32 devices in a mesh: sp: 8 (over z, x), tp: 4 (over y, core).
Axes of the slice: x: 2, y: 2, z: 4, core: 2. Of those that a mesh axis runs over, the one named last changes fastest.
Arguments:
- queries: bfloat16 [4096, 512], P('sp', 'tp'), may hold values from -16 to 16
- key_heads: bfloat16 [4096, 512], P('sp', 'tp'), may hold values from -16 to 16
- value_heads: bfloat16 [4096, 512], P('sp', 'tp'), may hold values from -6 to 6
- head_gain: float32 [512], P('tp'), may hold values from 0.1 to 1.9
- residual: bfloat16 [4096, 2048], P(('sp', 'tp')), may hold values from -6 to 6
- out_weight: bfloat16 [512, 2048], replicated, may hold values from -0.25 to 0.25
- norm_gain: float32 [2048], replicated, may hold values from 0.1 to 1.9
- shared_gate: bfloat16 [2048, 512], replicated, may hold values from -0.125 to 0.125
- shared_up: bfloat16 [2048, 512], replicated, may hold values from -0.125 to 0.125
- shared_down: bfloat16 [512, 2048], replicated, may hold values from -0.25 to 0.25
- expert_gate: bfloat16 [64, 2048, 512], P(('sp', 'tp')), may hold values from -0.125 to 0.125
- expert_up: bfloat16 [64, 2048, 512], P(('sp', 'tp')), may hold values from -0.125 to 0.125
- expert_down: bfloat16 [64, 512, 2048], P(('sp', 'tp')), may hold values from -0.25 to 0.25
- routed_experts: int32 [4096, 4], P(('sp', 'tp')), may hold values from 0 to 63, all different within a row; in each aligned block of 128 rows (0 to 127, 128 to 255, ...) at most 12 rows name the same one
- route_weights: float32 [4096, 4], P(('sp', 'tp')), may hold values from 0.1 to 1.5
Outputs:
- layer_output: bfloat16 [4096, 2048], P(('sp', 'tp'))
The draws below stay inside these ranges and needn't reach their ends.
Inputs may be any that keep to these rules, and one draw needn't show every extreme that they name: `routed_experts`: each row names 4 different experts. Within the rows of one device (128 consecutive rows, aligned) no expert is named more than 12 times, and in every draw some expert is named exactly 12 times in some device's rows.
All inputs are finite; a program needn't handle non-finite values.
Results may differ from the reference program's by a relative error of at most 0.014.
Values may be sent and summed in bfloat16 or wider, within the bound.
A program may use at most 128 MiB of HBM per device.

```python
import math
import jax
import jax.numpy as jnp
import numpy as np
from jax import lax

D = 2048
HEADS = 8
HEAD_DIM = 64
FFE = 512
SHARED_FF = 512
TOPK = 4
TOK_DEV = 128
TOK_SP = 512
TOKEN_COUNT = 4096
EXPERTS = 64
CAP = 12
N_SP = 8
N_TP = 4


def head_law(key):
    base_key = jax.random.fold_in(key, 11)
    direction_key, choice_key, quick_key, gentle_key = jax.random.split(base_key, 4)
    direction = jax.random.normal(direction_key, (HEADS, HEAD_DIM), jnp.float32)
    direction = direction / jnp.sqrt(jnp.sum(direction * direction, axis=1, keepdims=True))
    gentle_share = 0.5
    gentle = jax.random.uniform(choice_key, (HEADS,), jnp.float32) < gentle_share
    quick_rate = jnp.exp(jax.random.uniform(quick_key, (HEADS,), jnp.float32, math.log(3.3), math.log(4.6)))
    gentle_rate = math.log(TOKEN_COUNT) + jax.random.uniform(gentle_key, (HEADS,), jnp.float32, 0.0, 0.8)
    intensity = jnp.where(gentle, gentle_rate, quick_rate)
    return (direction, intensity)


def draw_queries(key, part):
    direction, intensity = head_law(key)
    noise = jnp.clip(jax.random.normal(jax.random.fold_in(key, 21), (TOKEN_COUNT, HEADS, HEAD_DIM), jnp.float32), -3.0, 3.0)
    lifted = jnp.sqrt(intensity * math.sqrt(HEAD_DIM))
    drawn = 0.5 * noise + lifted[None, :, None] * direction[None]
    return drawn.reshape(TOKEN_COUNT, HEADS * HEAD_DIM).astype(jnp.bfloat16)


def draw_key_heads(key, part):
    direction, intensity = head_law(key)
    jitter_random_key, shift_random_key, spike_random_key = jax.random.split(jax.random.fold_in(key, 31), 3)
    noise = jnp.clip(jax.random.normal(jitter_random_key, (TOKEN_COUNT, HEADS, HEAD_DIM), jnp.float32), -3.0, 3.0)
    shift_values = jax.random.uniform(shift_random_key, (TOKEN_COUNT // TOK_SP,), jnp.float32, -0.5, 0.5)
    shift_values = jnp.repeat(shift_values, TOK_SP)
    spike_amount = jax.random.uniform(spike_random_key, (TOKEN_COUNT,), jnp.float32) < 6.0 / TOKEN_COUNT
    lifted = jnp.sqrt(intensity * math.sqrt(HEAD_DIM))
    multiplier = jnp.where(spike_amount[:, None], 0.8 / intensity[None, :], 1.0 + shift_values[:, None] / intensity[None, :])
    drawn = 0.5 * noise - (lifted[None, :] * multiplier)[:, :, None] * direction[None]
    return drawn.reshape(TOKEN_COUNT, HEADS * HEAD_DIM).astype(jnp.bfloat16)


def levels(rng, extent, cuts, least, high):
    factor_of, own = 1.0, jax.random.fold_in(rng, 6)
    for position, shards_of in cuts:
        heights = jnp.exp(jax.random.uniform(jax.random.fold_in(own, position), (shards_of,), jnp.float32, least / len(cuts), high / len(cuts)))
        factor_of = factor_of * jnp.repeat(heights, extent[position] // shards_of).reshape([-1 if axis == position else 1 for axis in range(len(extent))])
    return factor_of


def assign_block(key, own, number, rows, number_of, top, reach, skew):
    order = jax.random.permutation(key, number_of)
    heavy_load, usual = load_shares(number_of, rows * top, reach, skew, True), load_shares(number_of, rows * top, reach, skew, False)
    places = jnp.arange(number_of)

    def named(tallies, turn):
        used = int((tallies > 0).sum())
        fixed = max(1, used // 4)
        shifted = fixed + (places - fixed + turn * (used - fixed)) % max(1, number_of - fixed)
        return jnp.zeros((number_of,), jnp.int32).at[order[jnp.where(places < fixed, places, shifted)]].set(jnp.asarray(tallies, jnp.int32))

    tallies = jnp.where(number % 4 == 0, named(heavy_load, number // 4), named(usual, number - number // 4 - 1))
    mixed = jax.random.permutation(jax.random.fold_in(own, 3), number_of)
    source_of, receiver = mixed[0:number_of // 2 * 2:2], mixed[1:number_of // 2 * 2:2]
    room = jnp.minimum(tallies[source_of] - 1, reach - tallies[receiver]) // 2
    room = jnp.where((source_of == order[0]) | (receiver == order[0]) | (tallies[receiver] == 0), 0, jnp.maximum(room, 0))
    shifted = jax.random.randint(jax.random.fold_in(own, 4), (number_of // 2,), 0, 1 << 20) % (room + 1)
    tallies = tallies.at[source_of].add(-shifted).at[receiver].add(shifted)
    labels = jnp.searchsorted(jnp.cumsum(tallies), jnp.arange(rows * top), side="right").astype(jnp.int32)
    grid = labels.reshape(top, rows).T
    grid = grid[jax.random.permutation(jax.random.fold_in(own, 1), rows)]
    turn = jax.random.randint(jax.random.fold_in(own, 2), (rows, 1), 0, top)
    return jnp.take_along_axis(grid, (jnp.arange(top)[None, :] + turn) % top, axis=1)


def load_shares(number_of, total, bound, lean, full):
    loads = [(1 << 20) // math.isqrt(rank ** lean) + 1 for rank in range(1, number_of + 1)]
    largest = bound if full else min(bound, max(-(-total // number_of), total * loads[0] // sum(loads)))
    least = 1 if total - largest >= number_of - 1 else 0
    holding, rest = [largest] + [least] * (number_of - 1), total - largest - least * (number_of - 1)
    while rest > 0:
        free = [i for i in range(1, number_of) if holding[i] < largest] or [i for i in range(1, number_of) if holding[i] < bound]
        pool, left = sum([loads[i] for i in free]), rest
        for i in free:
            extra = min(bound - holding[i], max(1, left * loads[i] // pool), rest)
            holding[i] = holding[i] + extra
            rest = rest - extra
    return np.array(holding)


def gaussian(rng, extent, scale, limit, cuts=(), kind=jnp.bfloat16):
    result = scale * jax.random.normal(rng, extent, jnp.float32)
    if cuts:
        result = result * levels(rng, extent, cuts, -0.22, 0.18)
    return jnp.clip(result, -limit, limit).astype(kind)


def setup_inputs(seed: int = 0) -> dict:
    key_of = jax.random.split(jax.random.key(seed), 16)
    queries = draw_queries(jax.random.fold_in(key_of[15], 71), 0)
    key_heads = draw_key_heads(jax.random.fold_in(key_of[15], 71), 0)
    value_heads = gaussian(key_of[2], (TOKEN_COUNT, HEADS * HEAD_DIM), 1.0, 6.0, ((0, 8), (1, 4)))
    head_gain = jnp.clip(1.0 + 0.18 * jax.random.normal(key_of[3], (HEADS * HEAD_DIM,), jnp.float32), 0.1, 1.9)
    residual = gaussian(key_of[4], (TOKEN_COUNT, D), 1.0, 6.0, ((0, 32),))
    out_weight = gaussian(key_of[5], (HEADS * HEAD_DIM, D), (HEADS * HEAD_DIM) ** -0.5, 0.25)
    norm_gain = jnp.clip(1.0 + 0.18 * jax.random.normal(key_of[6], (D,), jnp.float32), 0.1, 1.9)
    shared_gate = gaussian(key_of[7], (D, SHARED_FF), D ** -0.5, 0.125)
    shared_up = gaussian(key_of[8], (D, SHARED_FF), D ** -0.5, 0.125)
    shared_down = gaussian(key_of[9], (SHARED_FF, D), SHARED_FF ** -0.5, 0.25)
    expert_gate = gaussian(key_of[10], (EXPERTS, D, FFE), D ** -0.5, 0.125, ((0, 32),))
    expert_up = gaussian(key_of[11], (EXPERTS, D, FFE), D ** -0.5, 0.125, ((0, 32),))
    expert_down = gaussian(key_of[12], (EXPERTS, FFE, D), FFE ** -0.5, 0.25, ((0, 32),))
    routed_experts_keys = jax.random.split(jax.random.fold_in(key_of[13], 1), TOKEN_COUNT // TOK_DEV)
    routed_experts_turns = jax.random.permutation(jax.random.fold_in(key_of[13], 3), TOKEN_COUNT // TOK_DEV)
    routed_experts = jax.vmap(lambda own, number: assign_block(jax.random.fold_in(key_of[13], 2), own, number, TOK_DEV, EXPERTS, TOPK, CAP, 2))(routed_experts_keys, routed_experts_turns).reshape((TOKEN_COUNT, TOPK))
    route_weights = jnp.clip(jnp.exp(math.log(1.5) - 2.7080502 * jax.random.uniform(key_of[14], (TOKEN_COUNT, TOPK), jnp.float32) ** levels(key_of[14], (TOKEN_COUNT, TOPK), ((0, 32),), -0.2, 0.2)), 0.1, 1.5)
    return dict(queries=queries, key_heads=key_heads, value_heads=value_heads, head_gain=head_gain, residual=residual, out_weight=out_weight, norm_gain=norm_gain, shared_gate=shared_gate, shared_up=shared_up, shared_down=shared_down, expert_gate=expert_gate, expert_up=expert_up, expert_down=expert_down, routed_experts=routed_experts, route_weights=route_weights)


EPSILON = 1e-06

def block_terms(query_block, key_block, value_block, query_start, key_start):
    scale = 1.0 / math.sqrt(HEAD_DIM)
    scores = jnp.einsum('qhd,khd->hqk', query_block.astype(jnp.float32), key_block.astype(jnp.float32)) * scale
    query_places = query_start + lax.iota(jnp.int32, query_block.shape[0])
    key_places = key_start + lax.iota(jnp.int32, key_block.shape[0])
    earlier = (key_places[None, :] < query_places[:, None])[None]
    stay_log = jnp.where(earlier, jax.nn.log_sigmoid(-scores), 0.0)
    after_log = lax.cumsum(stay_log, axis=2, reverse=True) - stay_log
    weights = jnp.where(earlier, jnp.exp(jax.nn.log_sigmoid(scores) + after_log), 0.0).astype(jnp.bfloat16)
    partial_out = jnp.einsum('hqk,khd->qhd', weights.astype(jnp.float32), value_block.astype(jnp.float32))
    block_total = jnp.transpose(lax.optimization_barrier(jnp.sum(stay_log, axis=2)))
    return (block_total, partial_out)

def head_norm(mixed, head_gain):
    inverse = lax.rsqrt(lax.optimization_barrier(jnp.mean(mixed * mixed, axis=2, keepdims=True)) + EPSILON)
    normed = mixed * inverse * head_gain.reshape(mixed.shape[1], mixed.shape[2])
    return normed.reshape(mixed.shape[0], -1).astype(jnp.bfloat16)

def stick_breaking(queries, key_heads, value_heads):
    query_width = 512 if TOK_SP % 512 == 0 else TOK_SP
    query_all = queries.reshape(TOKEN_COUNT // query_width, query_width, HEADS, HEAD_DIM)
    key_all = key_heads.reshape(N_SP, TOK_SP, HEADS, HEAD_DIM)
    value_all = value_heads.reshape(N_SP, TOK_SP, HEADS, HEAD_DIM)

    def one_block(block_index):
        query_block = lax.dynamic_index_in_dim(query_all, block_index, 0, keepdims=False)
        query_start = block_index * query_width

        def one_shard(running, shard_index):
            key_start = shard_index * TOK_SP

            def compute(unused):
                key_block = lax.dynamic_index_in_dim(key_all, shard_index, 0, keepdims=False)
                value_block = lax.dynamic_index_in_dim(value_all, shard_index, 0, keepdims=False)
                return block_terms(query_block, key_block, value_block, query_start, key_start)

            def nothing(unused):
                return (jnp.zeros((query_width, HEADS), jnp.float32), jnp.zeros((query_width, HEADS, HEAD_DIM), jnp.float32))
            return (running, lax.cond(key_start < query_start + query_width, compute, nothing, 0))
        leftover, stacked = lax.scan(one_shard, jnp.int32(0), jnp.arange(N_SP, dtype=jnp.int32))
        totals, partials = stacked
        later = lax.cumsum(totals, axis=0, reverse=True) - totals
        return lax.optimization_barrier(jnp.sum(jnp.exp(later)[..., None] * partials, axis=0))
    mixed = lax.map(one_block, jnp.arange(TOKEN_COUNT // query_width, dtype=jnp.int32))
    return mixed.reshape(TOKEN_COUNT, HEADS, HEAD_DIM)

def expert_block(inputs):
    expert_rows, gate_weight, up_weight, down_weight = inputs
    gate_part = jnp.dot(expert_rows, gate_weight, preferred_element_type=jnp.float32)
    up_part = jnp.dot(expert_rows, up_weight, preferred_element_type=jnp.float32)
    hidden = (jax.nn.silu(gate_part) * up_part).astype(jnp.bfloat16)
    return jnp.dot(hidden, down_weight, preferred_element_type=jnp.float32).astype(jnp.bfloat16)

def routed_sum(expert_input, expert_gate, expert_up, expert_down, routed_experts, route_weights):
    device_count = N_SP * N_TP
    flat_experts = routed_experts.reshape(-1)
    expert_table = (flat_experts[:, None] == jnp.arange(EXPERTS, dtype=jnp.int32)[None, :]).astype(jnp.int32)
    expert_table = expert_table.reshape(device_count, TOK_DEV * TOPK, EXPERTS)
    ranking = (lax.optimization_barrier(jnp.sum(jnp.cumsum(expert_table, axis=1) * expert_table, axis=2)) - 1).reshape(-1)
    source = jnp.arange(TOKEN_COUNT * TOPK, dtype=jnp.int32) // (TOK_DEV * TOPK)
    slot_index = (flat_experts * device_count + source) * CAP + ranking
    repeated = jnp.repeat(expert_input, TOPK, axis=0)
    buffer = jnp.zeros((EXPERTS * device_count * CAP, D), jnp.bfloat16).at[slot_index].set(repeated)
    buffer = buffer.reshape(EXPERTS, device_count * CAP, D)
    results = lax.map(expert_block, (buffer, expert_gate, expert_up, expert_down)).reshape(-1, D)
    slot_grid = slot_index.reshape(TOKEN_COUNT, TOPK)
    routed = jnp.zeros((TOKEN_COUNT, D), jnp.float32)
    for choice_index in range(TOPK):
        picked = results[slot_grid[:, choice_index]].astype(jnp.float32)
        routed = routed + picked * route_weights[:, choice_index][:, None]
    return routed

def reference(queries, key_heads, value_heads, head_gain, residual, out_weight, norm_gain, shared_gate, shared_up, shared_down, expert_gate, expert_up, expert_down, routed_experts, route_weights):
    head_output = head_norm(stick_breaking(queries, key_heads, value_heads), head_gain)
    branch = jnp.dot(head_output, out_weight, preferred_element_type=jnp.float32)
    stream = (residual.astype(jnp.float32) + branch).astype(jnp.bfloat16)
    stream_wide = stream.astype(jnp.float32)
    inverse = lax.rsqrt(lax.optimization_barrier(jnp.mean(stream_wide * stream_wide, axis=1, keepdims=True)) + EPSILON)
    expert_input = (stream_wide * inverse * norm_gain).astype(jnp.bfloat16)
    shared_hidden = (jax.nn.silu(jnp.dot(expert_input, shared_gate, preferred_element_type=jnp.float32)) * jnp.dot(expert_input, shared_up, preferred_element_type=jnp.float32)).astype(jnp.bfloat16)
    shared_term = jnp.dot(shared_hidden, shared_down, preferred_element_type=jnp.float32)
    routed = routed_sum(expert_input, expert_gate, expert_up, expert_down, routed_experts, route_weights)
    return (stream_wide + shared_term + routed).astype(jnp.bfloat16)
```

```python
import functools
import math

import jax
import jax.numpy as jnp
from jax import lax
from jax.experimental import pallas as pl
from jax.experimental.pallas import tpu as pltpu
from jax.sharding import PartitionSpec as P

HEAD_DIM = 64


EPSILON = 1e-06

COLUMNS = 2
TILE = 256
LOG2E = 1.4426950408889634
MESH = pl.DeviceIdType.MESH


def attention_kernel(rows, q_ref, kv_ref, gain_ref, out_ref, held, acc, carry, up_send, up_recv, side_send, side_recv):
    me = lax.axis_index("sp")
    row, col = me // COLUMNS, me % COLUMNS
    seq, width = q_ref.shape
    heads = width // HEAD_DIM
    tile = min(TILE, seq)
    tiles = seq // tile
    other = row * COLUMNS + (COLUMNS - 1 - col)

    barrier = pltpu.get_barrier_semaphore()

    @pl.when(row < rows - 1)
    def _():
        pl.semaphore_signal(barrier, inc=1, device_id={"sp": me + COLUMNS}, device_id_type=MESH)

    @pl.when(row > 0)
    def _():
        pl.semaphore_signal(barrier, inc=1, device_id={"sp": me - COLUMNS}, device_id_type=MESH)

    pl.semaphore_signal(barrier, inc=1, device_id={"sp": other}, device_id_type=MESH)
    inner = (row > 0) & (row < rows - 1)

    @pl.when(inner)
    def _():
        pl.semaphore_wait(barrier, 3)

    @pl.when(jnp.logical_not(inner))
    def _():
        pl.semaphore_wait(barrier, min(rows, 2))

    def up_copy(source, depth):
        place = (row - depth) * COLUMNS + col
        return pltpu.make_async_remote_copy(
            src_ref=source, dst_ref=held.at[place], send_sem=up_send.at[depth], recv_sem=up_recv.at[depth],
            device_id={"sp": me + COLUMNS}, device_id_type=MESH)

    def side_copy(source, depth):
        place = (row - depth) * COLUMNS + col
        return pltpu.make_async_remote_copy(
            src_ref=source, dst_ref=held.at[place], send_sem=side_send.at[depth], recv_sem=side_recv.at[depth],
            device_id={"sp": other}, device_id_type=MESH)

    @pl.when(row < rows - 1)
    def _():
        up_copy(kv_ref, 0).start()

    @pl.when(col == 0)
    def _():
        side_copy(kv_ref, 0).start()

    lane = lax.broadcasted_iota(jnp.int32, (1, width), 1) // HEAD_DIM
    key_row = lax.broadcasted_iota(jnp.int32, (tile, tile), 0)
    key_col = lax.broadcasted_iota(jnp.int32, (tile, tile), 1)
    later = (key_row > key_col).astype(jnp.bfloat16)
    scale = LOG2E / math.sqrt(HEAD_DIM)

    def one(source, key_tile, query_tile, head, diagonal):
        query_rows = slice(query_tile * tile, (query_tile + 1) * tile)
        key_rows = slice(key_tile * tile, (key_tile + 1) * tile)
        queries = jnp.where(lane == head, q_ref[query_rows, :], jnp.zeros((), q_ref.dtype))
        keys = source[key_rows, :width]
        values = source[key_rows, width:]
        scores = lax.dot_general(queries, keys, (((1,), (1,)), ((), ())), preferred_element_type=jnp.float32) * scale
        soft = jnp.log2(1.0 + jnp.exp2(-jnp.abs(scores)))
        take = jnp.minimum(scores, 0.0) - soft
        stay = take - scores
        if diagonal:
            stay = jnp.where(key_col < key_row, stay, 0.0)
        high = stay.astype(jnp.bfloat16)
        low = (stay - high.astype(jnp.float32)).astype(jnp.bfloat16)
        after = jnp.dot(high, later, preferred_element_type=jnp.float32) + jnp.dot(low, later, preferred_element_type=jnp.float32)
        before = carry[head, query_rows, :]
        weights = jnp.exp2(take + after + before)
        if diagonal:
            weights = jnp.where(key_col < key_row, weights, 0.0)
        part = jnp.dot(weights.astype(jnp.bfloat16), values, preferred_element_type=jnp.float32)
        acc[query_rows, :] += jnp.where(lane == head, part, 0.0)
        carry[head, query_rows, :] = before + (after[:, :1] + stay[:, :1])

    acc[...] = jnp.zeros_like(acc)
    carry[...] = jnp.zeros_like(carry)
    for key_tile in range(tiles - 1, -1, -1):
        for query_tile in range(key_tile, tiles):
            for head in range(heads):
                one(kv_ref, key_tile, query_tile, head, key_tile == query_tile)

    def receive(depth):
        place = (row - depth) * COLUMNS + col
        up_copy(held.at[place], depth - 1).wait_recv()

        @pl.when(row < rows - 1)
        def _():
            up_copy(held.at[place], depth).start()

        side_copy(held.at[place], depth).start()

    def step(index, unused):
        shard = me - 1 - index
        depth = row - shard // COLUMNS

        @pl.when(shard % COLUMNS != col)
        def _():
            @pl.when(depth + col <= row)
            def _():
                receive(depth + col)

            side_copy(held.at[shard], depth).wait_recv()

        source = held.at[shard]
        for key_tile in range(tiles - 1, -1, -1):
            for query_tile in range(tiles):
                for head in range(heads):
                    one(source, key_tile, query_tile, head, False)
        return unused

    lax.fori_loop(0, me, step, 0)

    def finish(depth, unused):
        @pl.when(row < rows - 1)
        def _():
            up_copy(kv_ref, depth).wait_send()

        @pl.when((col == 0) | (depth > 0))
        def _():
            side_copy(kv_ref, depth).wait_send()

        return unused

    lax.fori_loop(0, row + 1, finish, 0)

    mixed = acc[...]
    square = mixed * mixed
    inverse = jnp.zeros_like(mixed)
    for head in range(heads):
        mean = jnp.sum(jnp.where(lane == head, square, 0.0), axis=1, keepdims=True) * (1.0 / HEAD_DIM)
        inverse = jnp.where(lane == head, lax.rsqrt(mean + EPSILON), inverse)
    out_ref[...] = (mixed * inverse * gain_ref[...]).astype(out_ref.dtype)


def attention(queries, key_heads, value_heads, head_gain):
    seq, width = queries.shape
    shards = lax.axis_size("sp")
    rows = shards // COLUMNS
    heads = width // HEAD_DIM
    both = jnp.concatenate([key_heads, value_heads], axis=1)
    vmem = pl.BlockSpec(memory_space=pltpu.VMEM)
    return pl.pallas_call(
        functools.partial(attention_kernel, rows),
        out_shape=jax.ShapeDtypeStruct((seq, width), jnp.bfloat16),
        in_specs=[vmem] * 3,
        out_specs=vmem,
        scratch_shapes=[
            pltpu.VMEM((shards, seq, 2 * width), jnp.bfloat16),
            pltpu.VMEM((seq, width), jnp.float32),
            pltpu.VMEM((heads, seq, 1), jnp.float32),
            pltpu.SemaphoreType.DMA((rows,)),
            pltpu.SemaphoreType.DMA((rows,)),
            pltpu.SemaphoreType.DMA((rows,)),
            pltpu.SemaphoreType.DMA((rows,)),
        ],
        compiler_params=pltpu.CompilerParams(collective_id=0, has_side_effects=True),
        name="attention",
    )(queries, both, head_gain.reshape(1, width))


def round_up(value, unit):
    return (value + unit - 1) // unit * unit


def routed_sum(expert_input, expert_gate, expert_up, expert_down, routed_experts, route_weights):
    row_count, pick_count = routed_experts.shape
    local_experts = expert_gate.shape[0]
    model_width = expert_input.shape[1]
    device_count = lax.axis_size("sp") * lax.axis_size("tp")
    expert_count = local_experts * device_count
    capacity = max(2, 3 * row_count * pick_count // (2 * expert_count))
    span = round_up(local_experts * capacity, 8)
    flat_experts = routed_experts.reshape(-1)
    expert_table = (
        flat_experts[:, None] == jnp.arange(expert_count, dtype=jnp.int32)[None, :]
    ).astype(jnp.bfloat16)
    pick_row = lax.broadcasted_iota(jnp.int32, (flat_experts.shape[0],) * 2, 0)
    pick_col = lax.broadcasted_iota(jnp.int32, (flat_experts.shape[0],) * 2, 1)
    earlier = (pick_col < pick_row).astype(jnp.bfloat16)
    counts = jnp.dot(earlier, expert_table, preferred_element_type=jnp.float32)
    ranking = jnp.sum(counts * expert_table.astype(jnp.float32), axis=1).astype(jnp.int32)
    slot_index = (flat_experts // local_experts) * span + (flat_experts % local_experts) * capacity + ranking
    match = (
        slot_index.reshape(row_count, pick_count)[:, :, None]
        == jnp.arange(device_count * span, dtype=jnp.int32)[None, None, :]
    )
    token_place = jnp.sum(match.astype(jnp.float32), axis=1).astype(jnp.bfloat16)
    outgoing = jnp.einsum(
        "rs,rd->sd", token_place, expert_input, preferred_element_type=jnp.float32
    ).astype(jnp.bfloat16)
    outgoing = outgoing.reshape(device_count, span, model_width)
    arrived = lax.all_to_all(outgoing, ("sp", "tp"), split_axis=0, concat_axis=0, tiled=True)
    places = lax.broadcasted_iota(jnp.int32, (1, span, 1), 1)
    result = jnp.zeros(arrived.shape, jnp.bfloat16)
    for expert in range(local_experts):
        first = expert * capacity // 8 * 8
        last = round_up((expert + 1) * capacity, 8)
        grouped = arrived[:, first:last].reshape(-1, model_width)
        gate_part = jnp.dot(grouped, expert_gate[expert], preferred_element_type=jnp.float32)
        up_part = jnp.dot(grouped, expert_up[expert], preferred_element_type=jnp.float32)
        hidden = (jax.nn.silu(gate_part) * up_part).astype(jnp.bfloat16)
        down = jnp.dot(hidden, expert_down[expert], preferred_element_type=jnp.float32).astype(jnp.bfloat16)
        down = jnp.pad(down.reshape(device_count, last - first, model_width), ((0, 0), (first, span - last), (0, 0)))
        mine = (places >= expert * capacity) & (places < (expert + 1) * capacity)
        result = jnp.where(mine, down, result)
    returned = lax.all_to_all(result, ("sp", "tp"), split_axis=0, concat_axis=0, tiled=True)
    returned = returned.reshape(-1, model_width)
    token_weight = jnp.sum(jnp.where(match, route_weights[:, :, None], 0.0), axis=1)
    high = token_weight.astype(jnp.bfloat16)
    low = (token_weight - high.astype(jnp.float32)).astype(jnp.bfloat16)
    return jnp.dot(high, returned, preferred_element_type=jnp.float32) + jnp.dot(
        low, returned, preferred_element_type=jnp.float32
    )


def body(
    queries,
    key_heads,
    value_heads,
    head_gain,
    residual,
    out_weight,
    norm_gain,
    shared_gate,
    shared_up,
    shared_down,
    expert_gate,
    expert_up,
    expert_down,
    routed_experts,
    route_weights,
):
    head_output = attention(queries, key_heads, value_heads, head_gain)
    token_heads = lax.all_to_all(head_output, "tp", split_axis=0, concat_axis=1, tiled=True)
    branch = jnp.dot(token_heads, out_weight, preferred_element_type=jnp.float32)
    stream = (residual.astype(jnp.float32) + branch).astype(jnp.bfloat16)
    stream_wide = stream.astype(jnp.float32)
    inverse = lax.rsqrt(jnp.mean(stream_wide * stream_wide, axis=1, keepdims=True) + EPSILON)
    expert_input = (stream_wide * inverse * norm_gain).astype(jnp.bfloat16)
    shared_hidden = (
        jax.nn.silu(jnp.dot(expert_input, shared_gate, preferred_element_type=jnp.float32))
        * jnp.dot(expert_input, shared_up, preferred_element_type=jnp.float32)
    ).astype(jnp.bfloat16)
    shared_term = jnp.dot(shared_hidden, shared_down, preferred_element_type=jnp.float32)
    routed = routed_sum(
        expert_input, expert_gate, expert_up, expert_down, routed_experts, route_weights
    )
    return (stream_wide + shared_term + routed).astype(jnp.bfloat16)


def solution(mesh):
    return jax.shard_map(
        body,
        mesh=mesh,
        in_specs=(
            P("sp", "tp"),
            P("sp", "tp"),
            P("sp", "tp"),
            P("tp"),
            P(("sp", "tp"), None),
            P(),
            P(),
            P(),
            P(),
            P(),
            P(("sp", "tp"), None, None),
            P(("sp", "tp"), None, None),
            P(("sp", "tp"), None, None),
            P(("sp", "tp"), None),
            P(("sp", "tp"), None),
        ),
        out_specs=P(("sp", "tp"), None),
        check_vma=False,
    )
```

```python
import functools
import math

import jax
import jax.numpy as jnp
from jax import lax
from jax.experimental import pallas as pl
from jax.experimental.pallas import tpu as pltpu
from jax.sharding import PartitionSpec as P

HEAD_DIM = 64


EPSILON = 1e-06

COLUMNS = 2
TILE = 256
LOG2E = 1.4426950408889634
MESH = pl.DeviceIdType.MESH


def attention_kernel(rows, q_ref, kv_ref, gain_ref, out_ref, held, masked, acc, carry, up_send, up_recv, side_send, side_recv):
    me = lax.axis_index("sp")
    row, col = me // COLUMNS, me % COLUMNS
    seq, width = q_ref.shape
    heads = width // HEAD_DIM
    tile = min(TILE, seq)
    tiles = seq // tile
    other = row * COLUMNS + (COLUMNS - 1 - col)

    barrier = pltpu.get_barrier_semaphore()

    @pl.when(row < rows - 1)
    def _():
        pl.semaphore_signal(barrier, inc=1, device_id={"sp": me + COLUMNS}, device_id_type=MESH)

    @pl.when(row > 0)
    def _():
        pl.semaphore_signal(barrier, inc=1, device_id={"sp": me - COLUMNS}, device_id_type=MESH)

    pl.semaphore_signal(barrier, inc=1, device_id={"sp": other}, device_id_type=MESH)
    inner = (row > 0) & (row < rows - 1)

    @pl.when(inner)
    def _():
        pl.semaphore_wait(barrier, 3)

    @pl.when(jnp.logical_not(inner))
    def _():
        pl.semaphore_wait(barrier, min(rows, 2))

    def up_copy(source, depth):
        place = (row - depth) * COLUMNS + col
        return pltpu.make_async_remote_copy(
            src_ref=source, dst_ref=held.at[place], send_sem=up_send.at[depth], recv_sem=up_recv.at[depth],
            device_id={"sp": me + COLUMNS}, device_id_type=MESH)

    def side_copy(source, depth):
        place = (row - depth) * COLUMNS + col
        return pltpu.make_async_remote_copy(
            src_ref=source, dst_ref=held.at[place], send_sem=side_send.at[depth], recv_sem=side_recv.at[depth],
            device_id={"sp": other}, device_id_type=MESH)

    @pl.when(row < rows - 1)
    def _():
        up_copy(kv_ref, 0).start()

    @pl.when(col == 0)
    def _():
        side_copy(kv_ref, 0).start()

    lane = lax.broadcasted_iota(jnp.int32, (1, width), 1) // HEAD_DIM
    key_row = lax.broadcasted_iota(jnp.int32, (tile, tile), 0)
    key_col = lax.broadcasted_iota(jnp.int32, (tile, tile), 1)
    later = (key_row > key_col).astype(jnp.bfloat16)
    scale = LOG2E / math.sqrt(HEAD_DIM)

    for head in range(heads):
        for query_tile in range(tiles):
            source_rows = slice(query_tile * tile, (query_tile + 1) * tile)
            stacked_rows = slice((query_tile * heads + head) * tile, (query_tile * heads + head + 1) * tile)
            masked[stacked_rows, :] = jnp.where(lane == head, q_ref[source_rows, :], jnp.zeros((), q_ref.dtype))

    def span(source, key_tile, first, last, diagonal):
        stacked_rows = slice(first * heads * tile, last * heads * tile)
        key_rows = slice(key_tile * tile, (key_tile + 1) * tile)
        keys = source[key_rows, :width]
        values = source[key_rows, width:]
        scores = lax.dot_general(masked[stacked_rows, :], keys, (((1,), (1,)), ((), ())), preferred_element_type=jnp.float32) * scale
        soft = jnp.log2(1.0 + jnp.exp2(-jnp.abs(scores)))
        take = jnp.minimum(scores, 0.0) - soft
        stay = take - scores
        if diagonal:
            query_place = jnp.concatenate([key_row] * ((last - first) * heads), axis=0)
            key_place = jnp.concatenate([key_col] * ((last - first) * heads), axis=0)
            stay = jnp.where(key_place < query_place, stay, 0.0)
        high = stay.astype(jnp.bfloat16)
        low = (stay - high.astype(jnp.float32)).astype(jnp.bfloat16)
        after = jnp.dot(high, later, preferred_element_type=jnp.float32) + jnp.dot(low, later, preferred_element_type=jnp.float32)
        before = carry[stacked_rows, :]
        weights = jnp.exp2(take + after + before)
        if diagonal:
            weights = jnp.where(key_place < query_place, weights, 0.0)
        acc[stacked_rows, :] += jnp.dot(weights.astype(jnp.bfloat16), values, preferred_element_type=jnp.float32)
        carry[stacked_rows, :] = before + (after[:, :1] + stay[:, :1])

    acc[...] = jnp.zeros_like(acc)
    carry[...] = jnp.zeros_like(carry)
    for key_tile in range(tiles - 1, -1, -1):
        span(kv_ref, key_tile, key_tile, key_tile + 1, True)
        if key_tile + 1 < tiles:
            span(kv_ref, key_tile, key_tile + 1, tiles, False)

    def receive(depth):
        place = (row - depth) * COLUMNS + col
        up_copy(held.at[place], depth - 1).wait_recv()

        @pl.when(row < rows - 1)
        def _():
            up_copy(held.at[place], depth).start()

        side_copy(held.at[place], depth).start()

    def step(index, unused):
        shard = me - 1 - index
        depth = row - shard // COLUMNS

        @pl.when(shard % COLUMNS != col)
        def _():
            @pl.when(depth + col <= row)
            def _():
                receive(depth + col)

            side_copy(held.at[shard], depth).wait_recv()

        source = held.at[shard]
        for key_tile in range(tiles - 1, -1, -1):
            span(source, key_tile, 0, tiles, False)
        return unused

    lax.fori_loop(0, me, step, 0)

    def finish(depth, unused):
        @pl.when(row < rows - 1)
        def _():
            up_copy(kv_ref, depth).wait_send()

        @pl.when((col == 0) | (depth > 0))
        def _():
            side_copy(kv_ref, depth).wait_send()

        return unused

    lax.fori_loop(0, row + 1, finish, 0)

    for query_tile in range(tiles):
        mixed = jnp.zeros((tile, width), jnp.float32)
        inverse = jnp.zeros((tile, width), jnp.float32)
        for head in range(heads):
            place = (query_tile * heads + head) * tile
            own = jnp.where(lane == head, acc[place : place + tile, :], 0.0)
            mean = jnp.sum(own * own, axis=1, keepdims=True) * (1.0 / HEAD_DIM)
            mixed = mixed + own
            inverse = jnp.where(lane == head, lax.rsqrt(mean + EPSILON), inverse)
        out_ref[query_tile * tile : (query_tile + 1) * tile, :] = (mixed * inverse * gain_ref[...]).astype(out_ref.dtype)


def attention(queries, key_heads, value_heads, head_gain):
    seq, width = queries.shape
    shards = lax.axis_size("sp")
    rows = shards // COLUMNS
    heads = width // HEAD_DIM
    both = jnp.concatenate([key_heads, value_heads], axis=1)
    vmem = pl.BlockSpec(memory_space=pltpu.VMEM)
    return pl.pallas_call(
        functools.partial(attention_kernel, rows),
        out_shape=jax.ShapeDtypeStruct((seq, width), jnp.bfloat16),
        in_specs=[vmem] * 3,
        out_specs=vmem,
        scratch_shapes=[
            pltpu.VMEM((shards, seq, 2 * width), jnp.bfloat16),
            pltpu.VMEM((heads * seq, width), jnp.bfloat16),
            pltpu.VMEM((heads * seq, width), jnp.float32),
            pltpu.VMEM((heads * seq, 1), jnp.float32),
            pltpu.SemaphoreType.DMA((rows,)),
            pltpu.SemaphoreType.DMA((rows,)),
            pltpu.SemaphoreType.DMA((rows,)),
            pltpu.SemaphoreType.DMA((rows,)),
        ],
        compiler_params=pltpu.CompilerParams(collective_id=0, has_side_effects=True),
        name="attention",
    )(queries, both, head_gain.reshape(1, width))


def round_up(value, unit):
    return (value + unit - 1) // unit * unit


def routed_sum(expert_input, expert_gate, expert_up, expert_down, routed_experts, route_weights):
    row_count, pick_count = routed_experts.shape
    local_experts = expert_gate.shape[0]
    model_width = expert_input.shape[1]
    device_count = lax.axis_size("sp") * lax.axis_size("tp")
    expert_count = local_experts * device_count
    capacity = max(2, 3 * row_count * pick_count // (2 * expert_count))
    span = round_up(local_experts * capacity, 8)
    flat_experts = routed_experts.reshape(-1)
    expert_table = (
        flat_experts[:, None] == jnp.arange(expert_count, dtype=jnp.int32)[None, :]
    ).astype(jnp.bfloat16)
    pick_row = lax.broadcasted_iota(jnp.int32, (flat_experts.shape[0],) * 2, 0)
    pick_col = lax.broadcasted_iota(jnp.int32, (flat_experts.shape[0],) * 2, 1)
    earlier = (pick_col < pick_row).astype(jnp.bfloat16)
    counts = jnp.dot(earlier, expert_table, preferred_element_type=jnp.float32)
    ranking = jnp.sum(counts * expert_table.astype(jnp.float32), axis=1).astype(jnp.int32)
    slot_index = (flat_experts // local_experts) * span + (flat_experts % local_experts) * capacity + ranking
    match = (
        slot_index.reshape(row_count, pick_count)[:, :, None]
        == jnp.arange(device_count * span, dtype=jnp.int32)[None, None, :]
    )
    token_place = jnp.sum(match.astype(jnp.float32), axis=1).astype(jnp.bfloat16)
    outgoing = jnp.einsum(
        "rs,rd->sd", token_place, expert_input, preferred_element_type=jnp.float32
    ).astype(jnp.bfloat16)
    outgoing = outgoing.reshape(device_count, span, model_width)
    arrived = lax.all_to_all(outgoing, ("sp", "tp"), split_axis=0, concat_axis=0, tiled=True)
    places = lax.broadcasted_iota(jnp.int32, (1, span, 1), 1)
    result = jnp.zeros(arrived.shape, jnp.bfloat16)
    for expert in range(local_experts):
        first = expert * capacity // 8 * 8
        last = round_up((expert + 1) * capacity, 8)
        grouped = arrived[:, first:last].reshape(-1, model_width)
        gate_part = jnp.dot(grouped, expert_gate[expert], preferred_element_type=jnp.float32)
        up_part = jnp.dot(grouped, expert_up[expert], preferred_element_type=jnp.float32)
        hidden = (jax.nn.silu(gate_part) * up_part).astype(jnp.bfloat16)
        down = jnp.dot(hidden, expert_down[expert], preferred_element_type=jnp.float32).astype(jnp.bfloat16)
        down = jnp.pad(down.reshape(device_count, last - first, model_width), ((0, 0), (first, span - last), (0, 0)))
        mine = (places >= expert * capacity) & (places < (expert + 1) * capacity)
        result = jnp.where(mine, down, result)
    returned = lax.all_to_all(result, ("sp", "tp"), split_axis=0, concat_axis=0, tiled=True)
    returned = returned.reshape(-1, model_width)
    token_weight = jnp.sum(jnp.where(match, route_weights[:, :, None], 0.0), axis=1)
    high = token_weight.astype(jnp.bfloat16)
    low = (token_weight - high.astype(jnp.float32)).astype(jnp.bfloat16)
    both = jnp.dot(jnp.concatenate([high, low], axis=0), returned, preferred_element_type=jnp.float32)
    return both[:row_count] + both[row_count:]


def body(
    queries,
    key_heads,
    value_heads,
    head_gain,
    residual,
    out_weight,
    norm_gain,
    shared_gate,
    shared_up,
    shared_down,
    expert_gate,
    expert_up,
    expert_down,
    routed_experts,
    route_weights,
):
    head_output = attention(queries, key_heads, value_heads, head_gain)
    token_heads = lax.all_to_all(head_output, "tp", split_axis=0, concat_axis=1, tiled=True)
    branch = jnp.dot(token_heads, out_weight, preferred_element_type=jnp.float32)
    stream = (residual.astype(jnp.float32) + branch).astype(jnp.bfloat16)
    stream_wide = stream.astype(jnp.float32)
    inverse = lax.rsqrt(jnp.mean(stream_wide * stream_wide, axis=1, keepdims=True) + EPSILON)
    expert_input = (stream_wide * inverse * norm_gain).astype(jnp.bfloat16)
    shared_hidden = (
        jax.nn.silu(jnp.dot(expert_input, shared_gate, preferred_element_type=jnp.float32))
        * jnp.dot(expert_input, shared_up, preferred_element_type=jnp.float32)
    ).astype(jnp.bfloat16)
    shared_term = jnp.dot(shared_hidden, shared_down, preferred_element_type=jnp.float32)
    routed = routed_sum(
        expert_input, expert_gate, expert_up, expert_down, routed_experts, route_weights
    )
    return (stream_wide + shared_term + routed).astype(jnp.bfloat16)


def solution(mesh):
    return jax.shard_map(
        body,
        mesh=mesh,
        in_specs=(
            P("sp", "tp"),
            P("sp", "tp"),
            P("sp", "tp"),
            P("tp"),
            P(("sp", "tp"), None),
            P(),
            P(),
            P(),
            P(),
            P(),
            P(("sp", "tp"), None, None),
            P(("sp", "tp"), None, None),
            P(("sp", "tp"), None, None),
            P(("sp", "tp"), None),
            P(("sp", "tp"), None),
        ),
        out_specs=P(("sp", "tp"), None),
        check_vma=False,
    )
```
